1024 devices in a mesh: fs: 32 (over z, core), tp: 32 (over y, x).
Axes of the slice: x: 4, y: 8, z: 16, core: 2. Of those that a mesh axis runs over, the one named last changes fastest.
Arguments:
- latent: bfloat16 [65536, 1024], P('fs'), may hold values from -6 to 6
- key_cotangent: bfloat16 [65536, 4096], P('fs', 'tp'), may hold values from -0.0234375 to 0.0234375
- value_cotangent: bfloat16 [65536, 4096], P('fs', 'tp'), may hold values from -0.0234375 to 0.0234375
- key_weight: float32 [1024, 4096], P('fs', 'tp'), may hold values from -50 to 50
- value_weight: float32 [1024, 4096], P('fs', 'tp'), may hold values from -50 to 50
- key_projector: bfloat16 [1024, 256], replicated, may hold values from -0.1875 to 0.1875
- value_projector: bfloat16 [1024, 256], replicated, may hold values from -0.1875 to 0.1875
- key_first: float32 [256, 4096], P(None, 'tp'), may hold values from -6 to 6
- key_second: float32 [256, 4096], P(None, 'tp'), may hold values from 0.3 to 3
- value_first: float32 [256, 4096], P(None, 'tp'), may hold values from -6 to 6
- value_second: float32 [256, 4096], P(None, 'tp'), may hold values from 0.3 to 3
Outputs:
- key_renewed: float32 [1024, 4096], P('fs', 'tp')
- value_renewed: float32 [1024, 4096], P('fs', 'tp')
- key_step: float32 [1024, 4096], P('fs', 'tp')
- value_step: float32 [1024, 4096], P('fs', 'tp')
- key_first_new: float32 [256, 4096], P(None, 'tp')
- key_second_new: float32 [256, 4096], P(None, 'tp')
- value_first_new: float32 [256, 4096], P(None, 'tp')
- value_second_new: float32 [256, 4096], P(None, 'tp')
- key_copy: bfloat16 [1024, 4096], P(None, 'tp')
- value_copy: bfloat16 [1024, 4096], P(None, 'tp')
The draws below stay inside these ranges and needn't reach their ends.
All inputs are finite; a program needn't handle non-finite values.
Results may differ from the reference program's by a relative error of at most 0.015.
Values may be sent and summed in bfloat16 or wider, within the bound.
No kernel may reach another device: no remote copies, remote signals or barrier semaphores. Data moves between devices by JAX's collectives and lax.ppermute only.
A program may use at most 32 MiB of HBM per device.

```python
import math
import jax
import jax.numpy as jnp
from jax import lax

LATENT_WIDTH = 1024
KEY_FEATURES = 128
VALUE_FEATURES = 128
FACTOR_RANK = 256
ATTENTION_HEADS = 32
TOKEN_COUNT = 65536
KEY_COLS = 4096
VALUE_COLS = 4096


def draw_weight_common(key, row_total, col_total):
    row_place = jnp.arange(row_total, dtype=jnp.float32) / row_total
    col_place = jnp.arange(col_total, dtype=jnp.float32) / col_total
    keys = jax.random.split(key, 3)
    row_scale = 10.0 ** row_place
    col_scale = 10.0 ** col_place
    values = jnp.clip(jax.random.normal(keys[2], (row_total, col_total), jnp.float32), -5.0, 5.0)
    return (values * jnp.sqrt(row_scale[:, None] * col_scale[None, :])).astype(jnp.float32)


def draw_key_weight(key, part):
    return draw_weight_common(jax.random.fold_in(key, 11), LATENT_WIDTH, ATTENTION_HEADS * KEY_FEATURES)


def draw_value_weight(key, part):
    return draw_weight_common(jax.random.fold_in(key, 23), LATENT_WIDTH, ATTENTION_HEADS * VALUE_FEATURES)


def strengthened(entries, key, source, target, shards_of, factor):
    owner, partner = [(jnp.arange(entries.shape[position]) // (entries.shape[position] // shards_of)).reshape([-1 if axis == position else 1 for axis in range(entries.ndim)]) for position in (source, target)]
    chosen = jax.random.permutation(key, shards_of)[partner]
    strong = (owner == chosen) | (owner == (partner + shards_of // 2) % shards_of)
    return jnp.where(strong, factor * entries, entries)


def levels(rng, extent, shards, smallest, top_value):
    gain, own = 1.0, jax.random.fold_in(rng, 6)
    for axis_at, parts in shards:
        heights = jnp.exp(jax.random.uniform(jax.random.fold_in(own, axis_at), (parts,), jnp.float32, smallest / len(shards), top_value / len(shards)))
        gain = gain * jnp.repeat(heights, extent[axis_at] // parts).reshape([-1 if axis == axis_at else 1 for axis in range(len(extent))])
    return gain


def noise(stream_key, shape, spread, reach, cuts=(), kind=jnp.bfloat16):
    entries = jax.random.normal(stream_key, shape, jnp.float32) * spread
    if len(cuts) > 0:
        entries = levels(stream_key, shape, cuts, -0.22, 0.18) * entries
    return jnp.clip(entries, min=-reach, max=reach).astype(kind)


def heavy_noise(own_key, extent, scale, most, pieces, heavy, held_as=jnp.bfloat16):
    array = scale * jax.random.normal(own_key, extent, jnp.float32)
    if pieces:
        array = array * levels(own_key, extent, pieces, -0.22, 0.18)
    return jnp.clip(strengthened(array, jax.random.fold_in(own_key, 3), *heavy), -most, most).astype(held_as)


def setup_inputs(seed: int = 0) -> dict:
    splits = jax.random.split(jax.random.key(seed), 12)
    return {
        "latent": heavy_noise(splits[0], (TOKEN_COUNT, LATENT_WIDTH), 1.0, 6.0, ((0, 32),), (0, 1, 32, 2.75)),
        "key_cotangent": noise(splits[1], (TOKEN_COUNT, KEY_COLS), (1.0 / TOKEN_COUNT ** 0.5), 0.0234375, ((0, 32), (1, 32))),
        "value_cotangent": noise(splits[2], (TOKEN_COUNT, VALUE_COLS), (1.0 / TOKEN_COUNT ** 0.5), 0.0234375, ((0, 32), (1, 32))),
        "key_weight": draw_key_weight(jax.random.fold_in(splits[11], 71), 0),
        "value_weight": draw_value_weight(jax.random.fold_in(splits[11], 71), 0),
        "key_projector": noise(splits[5], (LATENT_WIDTH, FACTOR_RANK), LATENT_WIDTH ** -0.5, 0.1875),
        "value_projector": noise(splits[6], (LATENT_WIDTH, FACTOR_RANK), LATENT_WIDTH ** -0.5, 0.1875),
        "key_first": noise(splits[7], (FACTOR_RANK, KEY_COLS), 1.0, 6.0, ((1, 32),), jnp.float32),
        "key_second": jnp.clip(jnp.exp(math.log(3.0) - 2.3025851 * jax.random.uniform(splits[8], (FACTOR_RANK, KEY_COLS), jnp.float32) ** levels(splits[8], (FACTOR_RANK, KEY_COLS), ((1, 32),), -0.2, 0.2)), 0.3, 3.0),
        "value_first": noise(splits[9], (FACTOR_RANK, VALUE_COLS), 1.0, 6.0, ((1, 32),), jnp.float32),
        "value_second": jnp.clip(jnp.exp(math.log(3.0) - 2.3025851 * jax.random.uniform(splits[10], (FACTOR_RANK, VALUE_COLS), jnp.float32) ** levels(splits[10], (FACTOR_RANK, VALUE_COLS), ((1, 32),), -0.2, 0.2)), 0.3, 3.0),
    }


EPSILON = 1e-08
FIRST_DECAY = 0.7
SECOND_DECAY = 0.8
LEARN_RATE = 0.2

def update(latent, weight, factor, cotangent, first_moment, second):
    reduced = jnp.dot(latent.astype(jnp.float32), factor.astype(jnp.float32), precision=lax.Precision.HIGHEST)
    projected = jnp.dot(reduced.T, cotangent.astype(jnp.float32), precision=lax.Precision.HIGHEST)
    first_new = FIRST_DECAY * first_moment + (1.0 - FIRST_DECAY) * projected
    second_new = SECOND_DECAY * second + (1.0 - SECOND_DECAY) * projected * projected
    normalized = first_new / (jnp.sqrt(second_new) + EPSILON)
    direction = jnp.dot(factor.astype(jnp.float32), normalized, precision=lax.Precision.HIGHEST)
    step_scale = LEARN_RATE * jnp.sqrt(jnp.mean(weight * weight))
    weight_step = step_scale * direction
    renewed = weight - weight_step
    return (renewed, weight_step, first_new, second_new, renewed.astype(jnp.bfloat16))

def reference(latent, key_cotangent, value_cotangent, key_weight, value_weight, key_projector, value_projector, key_first, key_second, value_first, value_second):
    key_out = update(latent, key_weight, key_projector, key_cotangent, key_first, key_second)
    value_out = update(latent, value_weight, value_projector, value_cotangent, value_first, value_second)
    return (key_out[0], value_out[0], key_out[1], value_out[1], key_out[2], key_out[3], value_out[2], value_out[3], key_out[4], value_out[4])
```

```python
import jax
import jax.numpy as jnp
from jax import lax
from jax.experimental import pallas as pl
from jax.experimental.pallas import tpu as pltpu
from jax.sharding import Mesh
from jax.sharding import PartitionSpec as P

Z, CORE = "fs_0", "fs_1"
FS = (Z, CORE)
TP = ("tp_0", "tp_1")

EPSILON = 1e-08
FIRST_DECAY = 0.7
SECOND_DECAY = 0.8
LEARN_RATE = 0.2

BF16, F32 = jnp.bfloat16, jnp.float32


def halves(x):
    high = x.astype(BF16)
    return high, (x - high.astype(F32)).astype(BF16)


def thirds(x):
    high = x.astype(BF16)
    rest = x - high.astype(F32)
    return (high,) + halves(rest)


def squares_kernel(key_ref, value_ref, out_ref):
    totals = [jnp.sum(r[...] * r[...]) for r in (key_ref, value_ref)]
    row = lax.broadcasted_iota(jnp.int32, out_ref.shape, 1)
    out_ref[...] = jnp.where(row == 0, totals[0], totals[1])


def project_kernel(core_ref, latent_ref, key_ref, value_ref, key_proj, value_proj, keep_ref, send_ref, acc_ref):
    step = pl.program_id(0)
    both = jnp.concatenate([key_ref[...], value_ref[...]], axis=1)
    part = lax.dot_general(both, latent_ref[...], (((0,), (0,)), ((), ())), preferred_element_type=F32)

    @pl.when(step == 0)
    def _():
        acc_ref[...] = part

    @pl.when(step > 0)
    def _():
        acc_ref[...] += part

    @pl.when(step == pl.num_programs(0) - 1)
    def _():
        results = []
        cols = key_ref.shape[1]
        for at, proj in ((0, key_proj), (cols, value_proj)):
            high, low = halves(acc_ref[at : at + cols, :])
            p = proj[...]
            r = jnp.dot(high, p, preferred_element_type=F32) + jnp.dot(low, p, preferred_element_type=F32)
            results.append(r.T)
        first = core_ref[0] == 0
        keep_ref[...] = jnp.where(first, results[0], results[1])
        send_ref[...] = jnp.where(first, results[1], results[0]).astype(BF16)


def spread_kernel(pieces_ref, key_ref, value_ref, squares_ref, out_ref):
    rows = pieces_ref.shape[1]
    total = jnp.sum(pieces_ref[...].astype(F32), axis=0).astype(BF16)
    squares = jnp.sum(squares_ref[...], axis=0)
    scalars = [t[0:1] for t in thirds(squares)] + [t[1:2] for t in thirds(squares)]
    scalars += [jnp.zeros((2, total.shape[1]), BF16)]
    message = jnp.concatenate(
        [total, key_ref[...].astype(BF16), value_ref[...].astype(BF16)], axis=0
    )
    tail = jnp.concatenate([s.astype(F32) for s in scalars], axis=0).astype(BF16)
    at = message.shape[0]
    for i in range(out_ref.shape[0]):
        out_ref[i, :at] = message
        out_ref[i, at:] = tail


def update_kernel(
    place_ref, data_ref, key_w, value_w, key_proj, value_proj, kf, ks, vf, vs,
    key_renewed, value_renewed, key_step, value_step,
    kf_new, ks_new, vf_new, vs_new, key_copy, value_copy,
    *, rows, weight_rows, entries,
):
    own = pl.multiple_of(place_ref[0] * weight_rows, weight_rows)
    cores, chips = data_ref.shape[0], data_ref.shape[1]
    tail = rows + 2 * weight_rows
    for which, (w, proj, first, second, renewed, step, first_new, second_new, copy) in enumerate((
        (key_w, key_proj, kf, ks, key_renewed, key_step, kf_new, ks_new, key_copy),
        (value_w, value_proj, vf, vs, value_renewed, value_step, vf_new, vs_new, value_copy),
    )):
        projected = data_ref[which, :, :rows, :].reshape(chips * rows, w.shape[1]).astype(F32)
        fn = FIRST_DECAY * first[...] + (1.0 - FIRST_DECAY) * projected
        sn = SECOND_DECAY * second[...] + (1.0 - SECOND_DECAY) * projected * projected
        first_new[...] = fn
        second_new[...] = sn
        pair = jnp.concatenate(halves(fn / (jnp.sqrt(sn) + EPSILON)), axis=1)
        sums = data_ref[:, :, tail:, :].astype(F32).sum(axis=(0, 1))
        total = sums[3 * which : 3 * which + 1] + sums[3 * which + 1 : 3 * which + 2] + sums[3 * which + 2 : 3 * which + 3]
        scale = LEARN_RATE * jnp.sqrt(total / entries)
        cols = w.shape[1]

        def steps_of(factor):
            r = jnp.dot(factor, pair, preferred_element_type=F32)
            return scale * (r[:, :cols] + r[:, cols:])

        mine = steps_of(proj[pl.ds(own, weight_rows), :])
        step[...] = mine
        renewed[...] = w[...] - mine
        everyone = steps_of(proj[...])
        at = rows + which * weight_rows
        for chip in range(chips):
            for core in range(cores):
                r = (chip * cores + core) * weight_rows
                old = data_ref[core, chip, at : at + weight_rows, :].astype(F32)
                copy[r : r + weight_rows, :] = (old - everyone[r : r + weight_rows]).astype(BF16)


def whole(a):
    return pl.BlockSpec(memory_space=pltpu.VMEM)


def body(
    latent, key_cotangent, value_cotangent, key_weight, value_weight,
    key_projector, value_projector, key_first, key_second, value_first, value_second,
):
    chips, cores = lax.axis_size(Z), lax.axis_size(CORE)
    columns = lax.axis_size(TP)
    weight_rows, cols = key_weight.shape
    tokens, width = latent.shape
    rank = key_projector.shape[1]
    core = lax.axis_index(CORE).astype(jnp.int32)
    place = lax.axis_index(FS).astype(jnp.int32)
    sds = jax.ShapeDtypeStruct
    smem = pl.BlockSpec(memory_space=pltpu.SMEM)
    vmem = pl.BlockSpec(memory_space=pltpu.VMEM)

    squares = pl.pallas_call(
        squares_kernel, out_shape=sds((columns, 8, 128), F32),
        in_specs=[vmem, vmem], out_specs=vmem, name="squares",
    )(key_weight, value_weight)
    squares = lax.all_to_all(squares, TP, 0, 0)

    block = min(tokens, 512)
    keep, send = pl.pallas_call(
        project_kernel,
        grid=(tokens // block,),
        out_shape=(sds((rank, cols), F32), sds((rank, cols), BF16)),
        in_specs=[
            smem,
            pl.BlockSpec((block, width), lambda i: (i, 0)),
            pl.BlockSpec((block, cols), lambda i: (i, 0)),
            pl.BlockSpec((block, cols), lambda i: (i, 0)),
            pl.BlockSpec((width, rank), lambda i: (0, 0)),
            pl.BlockSpec((width, rank), lambda i: (0, 0)),
        ],
        out_specs=(pl.BlockSpec((rank, cols), lambda i: (0, 0)),) * 2,
        scratch_shapes=[pltpu.VMEM((2 * cols, width), F32)],
        cost_estimate=pl.CostEstimate(flops=2_000_000_000, bytes_accessed=6_000_000, transcendentals=0),
        name="project",
    )(core.reshape(1), latent, key_cotangent, value_cotangent, key_projector, value_projector)

    other = lax.ppermute(send, CORE, [(0, 1), (1, 0)])
    rows = rank // chips
    pieces = (keep + other.astype(F32)).astype(BF16).reshape(chips, rows, cols)
    pieces = lax.all_to_all(pieces, Z, 0, 0)

    length = rows + 2 * weight_rows + 8
    message = pl.pallas_call(
        spread_kernel, out_shape=sds((chips, length, cols), BF16),
        in_specs=[vmem] * 4, out_specs=vmem, name="spread",
    )(pieces, key_weight, value_weight, squares)
    message = lax.all_to_all(message, Z, 0, 0)
    data = lax.all_gather(message, CORE)

    entries = float(key_weight.size * chips * cores * columns)
    weight = sds((weight_rows, cols), F32)
    moment = sds((rank, cols), F32)
    copy = sds((width, cols), BF16)

    def update(*refs):
        update_kernel(*refs, rows=rows, weight_rows=weight_rows, entries=entries)

    return pl.pallas_call(
        update,
        out_shape=(weight,) * 4 + (moment,) * 4 + (copy,) * 2,
        in_specs=[smem] + [vmem] * 9, out_specs=(vmem,) * 10, name="update",
    )(
        place.reshape(1), data, key_weight, value_weight, key_projector, value_projector,
        key_first, key_second, value_first, value_second,
    )


def solution(mesh):
    finer = Mesh(mesh.devices.reshape(16, 2, 8, 4), ("fs_0", "fs_1", "tp_0", "tp_1"))
    return jax.shard_map(
        body,
        mesh=finer,
        in_specs=(P(FS, None),) + (P(FS, TP),) * 4 + (P(),) * 2 + (P(None, TP),) * 4,
        out_specs=(P(FS, TP),) * 4 + (P(None, TP),) * 6,
        check_vma=False,
    )
```

```python
import jax
import jax.numpy as jnp
from jax import lax
from jax.experimental import pallas as pl
from jax.experimental.pallas import tpu as pltpu
from jax.sharding import Mesh
from jax.sharding import PartitionSpec as P


Z, CORE = "fs_0", "fs_1"
FS = (Z, CORE)
TP = ("tp_0", "tp_1")

EPSILON = 1e-08
FIRST_DECAY = 0.7
SECOND_DECAY = 0.8
LEARN_RATE = 0.2
LEAD = 0
TAIL = 8

BF16, F32 = jnp.bfloat16, jnp.float32


def halves(x):
    high = x.astype(BF16)
    return high, (x - high.astype(F32)).astype(BF16)


def tail_of(x, cols):
    row = lax.broadcasted_iota(jnp.int32, (TAIL, cols), 0)
    x = jnp.broadcast_to(x, (TAIL, cols))
    high = x.astype(BF16).astype(F32)
    mid = (x - high).astype(BF16).astype(F32)
    low = x - high - mid
    x = jnp.where(row == 0, high, jnp.where(row == 1, mid, jnp.where(row == 2, low, 0.0)))
    return x.astype(BF16)


def squares_kernel(key_ref, value_ref, out_ref):
    row = lax.broadcasted_iota(jnp.int32, out_ref.shape, 1)
    out_ref[...] = jnp.where(row == 0, jnp.sum(key_ref[...] * key_ref[...]), jnp.sum(value_ref[...] * value_ref[...]))


def project_kernel(
    latent_hbm, key_hbm, value_hbm, key_proj_hbm, value_proj_hbm, out_ref,
    latent, key, value, key_proj, value_proj, acc_ref, sems,
):
    chunks = sems.shape[0] - 4
    tokens = latent.shape[0] // chunks
    cols = key.shape[1]
    sides = [
        pltpu.make_async_copy(src, dst, sems.at[chunks + i])
        for i, (src, dst) in enumerate((
            (key_hbm, key), (value_hbm, value), (key_proj_hbm, key_proj), (value_proj_hbm, value_proj)
        ))
    ]
    mains = [
        pltpu.make_async_copy(
            latent_hbm.at[pl.ds(i * tokens, tokens)], latent.at[pl.ds(i * tokens, tokens)], sems.at[i]
        )
        for i in range(chunks)
    ]
    for copy in sides[:2] + mains + sides[2:]:
        copy.start()
    sides[0].wait()
    sides[1].wait()
    for i in range(chunks):
        mains[i].wait()
        at = slice(i * tokens, (i + 1) * tokens)
        both = jnp.concatenate([key[at, :], value[at, :]], axis=1)
        part = lax.dot_general(both, latent[at, :], (((0,), (0,)), ((), ())), preferred_element_type=F32)
        acc_ref[...] = part if i == 0 else acc_ref[...] + part
    for which, proj in enumerate((key_proj, value_proj)):
        sides[2 + which].wait()
        high, low = halves(acc_ref[which * cols : (which + 1) * cols])
        p = proj[...]
        r = jnp.dot(high, p, preferred_element_type=F32) + jnp.dot(low, p, preferred_element_type=F32)
        out_ref[which] = r.T.astype(BF16)


def cut_kernel(core_ref, parts_ref, squares_ref, out_ref):
    chips, length, cols = out_ref.shape
    rows = length - TAIL
    mine = parts_ref[:, core_ref[0]].astype(F32).sum(axis=0)
    out_ref[:, :rows] = mine.astype(BF16).reshape(chips, rows, cols)
    squares = jnp.sum(squares_ref[...], axis=0)
    row = lax.broadcasted_iota(jnp.int32, (TAIL, cols), 0)
    key = tail_of(squares[0:1], cols).astype(F32)
    value = tail_of(squares[1:2], cols).astype(F32)
    tail = jnp.where(row < TAIL // 2, key, pltpu.roll(value, TAIL // 2, 0)).astype(BF16)
    for i in range(chips):
        out_ref[i, rows:] = tail


def spread_kernel(pieces_ref, key_ref, value_ref, out_ref, squares_ref):
    rows = pieces_ref.shape[1] - TAIL
    total = jnp.sum(pieces_ref[...].astype(F32), axis=0)
    message = jnp.concatenate(
        [total[:rows].astype(BF16), key_ref[...].astype(BF16), value_ref[...].astype(BF16)], axis=0
    )
    for i in range(out_ref.shape[0]):
        out_ref[i] = message
    key = total[rows : rows + 1] + total[rows + 1 : rows + 2] + total[rows + 2 : rows + 3]
    rows += TAIL // 2
    value = total[rows : rows + 1] + total[rows + 1 : rows + 2] + total[rows + 2 : rows + 3]
    row = lax.broadcasted_iota(jnp.int32, squares_ref.shape, 0)
    squares_ref[...] = jnp.where(row == 0, key, value)


def update_kernel(
    place_ref, data_ref, squares_ref, key_w, value_w, key_proj, value_proj, kf, ks, vf, vs,
    key_renewed, value_renewed, key_step, value_step,
    kf_new, ks_new, vf_new, vs_new, key_copy, value_copy,
    *, rows, weight_rows, entries,
):
    own = pl.multiple_of(place_ref[0] * weight_rows, weight_rows)
    cores, chips = data_ref.shape[0], data_ref.shape[1]
    squares = squares_ref[...]
    for which, (w, proj, first, second, renewed, step, first_new, second_new, copy) in enumerate((
        (key_w, key_proj, kf, ks, key_renewed, key_step, kf_new, ks_new, key_copy),
        (value_w, value_proj, vf, vs, value_renewed, value_step, vf_new, vs_new, value_copy),
    )):
        projected = data_ref[which, :, :rows, :].reshape(chips * rows, w.shape[1]).astype(F32)
        fn = FIRST_DECAY * first[...] + (1.0 - FIRST_DECAY) * projected
        sn = SECOND_DECAY * second[...] + (1.0 - SECOND_DECAY) * projected * projected
        first_new[...] = fn
        second_new[...] = sn
        pair = jnp.concatenate(halves(fn / (jnp.sqrt(sn) + EPSILON)), axis=1)
        total = squares[which : which + 1]
        scale = LEARN_RATE * jnp.sqrt(total / entries)
        cols = w.shape[1]

        def steps_of(factor):
            r = jnp.dot(factor, pair, preferred_element_type=F32)
            return scale * (r[:, :cols] + r[:, cols:])

        mine = steps_of(proj[pl.ds(own, weight_rows), :])
        step[...] = mine
        renewed[...] = w[...] - mine
        everyone = steps_of(proj[...])
        at = rows + which * weight_rows
        for chip in range(chips):
            for core in range(cores):
                r = ((chip + LEAD) % chips * cores + core) * weight_rows
                old = data_ref[core, chip, at : at + weight_rows, :].astype(F32)
                copy[r : r + weight_rows, :] = (old - everyone[r : r + weight_rows]).astype(BF16)


def swap(a, chips):
    if LEAD == 0:
        return lax.all_to_all(a, Z, 0, 0)
    order = [(i + LEAD) % chips for i in range(chips)]
    return lax.all_to_all(a, Z, 0, 0, axis_index_groups=[order])


def near(a):
    return pltpu.with_memory_space_constraint(a, pltpu.VMEM)


def body(
    latent, key_cotangent, value_cotangent, key_weight, value_weight,
    key_projector, value_projector, key_first, key_second, value_first, value_second,
):
    chips, cores = lax.axis_size(Z), lax.axis_size(CORE)
    columns = lax.axis_size(TP)
    weight_rows, cols = key_weight.shape
    tokens, width = latent.shape
    rank = key_projector.shape[1]
    core = lax.axis_index(CORE).astype(jnp.int32)
    place = lax.axis_index(FS).astype(jnp.int32)
    sds = jax.ShapeDtypeStruct
    smem = pl.BlockSpec(memory_space=pltpu.SMEM)
    vmem = pl.BlockSpec(memory_space=pltpu.VMEM)

    squares = pl.pallas_call(
        squares_kernel, out_shape=(sds((cores * lax.axis_size(TP[1]), 8, cols), F32),),
        in_specs=[vmem, vmem], out_specs=(vmem,), name="squares",
    )(key_weight, value_weight)[0]
    squares = lax.all_to_all(squares, (CORE, TP[1]), 0, 0)
    parts = pl.pallas_call(
        project_kernel,
        out_shape=(pltpu.VMEM((2, rank, cols), BF16),),
        in_specs=[pl.BlockSpec(memory_space=pl.ANY)] * 5,
        out_specs=(vmem,),
        scratch_shapes=[
            pltpu.VMEM(latent.shape, BF16),
            pltpu.VMEM((tokens, cols), BF16),
            pltpu.VMEM((tokens, cols), BF16),
            pltpu.VMEM((width, rank), BF16),
            pltpu.VMEM((width, rank), BF16),
            pltpu.VMEM((2 * cols, width), F32),
            pltpu.SemaphoreType.DMA((8 + 4,)),
        ],
        name="project",
    )(latent, key_cotangent, value_cotangent, key_projector, value_projector)[0]
    parts = near(lax.all_gather(parts, CORE))

    rows = rank // chips
    pieces = pl.pallas_call(
        cut_kernel, out_shape=(pltpu.VMEM((chips, rows + TAIL, cols), BF16),),
        in_specs=[smem, vmem, vmem], out_specs=(vmem,), name="cut",
    )(core.reshape(1), parts, near(squares))[0]
    pieces = near(swap(pieces, chips))

    length = rows + 2 * weight_rows
    message, squares = pl.pallas_call(
        spread_kernel,
        out_shape=(pltpu.VMEM((chips, length, cols), BF16), pltpu.VMEM((8, cols), F32)),
        in_specs=[vmem] * 3, out_specs=(vmem, vmem), name="spread",
    )(pieces, near(key_weight), near(value_weight))
    message = swap(message, chips)
    squares = lax.psum(squares, TP[0])
    data = near(lax.all_gather(message, CORE))

    entries = float(key_weight.size * chips * cores * columns)
    weight = sds((weight_rows, cols), F32)
    moment = sds((rank, cols), F32)
    copy = sds((width, cols), BF16)

    def update(*refs):
        update_kernel(*refs, rows=rows, weight_rows=weight_rows, entries=entries)

    return pl.pallas_call(
        update,
        out_shape=(weight,) * 4 + (moment,) * 4 + (copy,) * 2,
        in_specs=[smem] + [vmem] * 10, out_specs=(vmem,) * 10, name="update",
    )(
        place.reshape(1), data, near(squares), *map(near, (
            key_weight, value_weight, key_projector, value_projector,
            key_first, key_second, value_first, value_second,
        ))
    )


def solution(mesh):
    finer = Mesh(mesh.devices.reshape(16, 2, 8, 4), ("fs_0", "fs_1", "tp_0", "tp_1"))
    return jax.shard_map(
        body,
        mesh=finer,
        in_specs=(P(FS, None),) + (P(FS, TP),) * 4 + (P(),) * 2 + (P(None, TP),) * 4,
        out_specs=(P(FS, TP),) * 4 + (P(None, TP),) * 6,
        check_vma=False,
    )
```

```python
import jax
import jax.numpy as jnp
from jax import lax
from jax.experimental import pallas as pl
from jax.experimental.pallas import tpu as pltpu
from jax.sharding import Mesh
from jax.sharding import PartitionSpec as P


Z, CORE = "fs_0", "fs_1"
FS = (Z, CORE)
TP = ("tp_0", "tp_1")

EPSILON = 1e-08
FIRST_DECAY = 0.7
SECOND_DECAY = 0.8
LEARN_RATE = 0.2
LEAD = 0
TAIL = 8

BF16, F32 = jnp.bfloat16, jnp.float32


def halves(x):
    high = x.astype(BF16)
    return high, (x - high.astype(F32)).astype(BF16)


def tail_of(x, cols):
    row = lax.broadcasted_iota(jnp.int32, (TAIL, cols), 0)
    x = jnp.broadcast_to(x, (TAIL, cols))
    high = x.astype(BF16).astype(F32)
    mid = (x - high).astype(BF16).astype(F32)
    low = x - high - mid
    x = jnp.where(row == 0, high, jnp.where(row == 1, mid, jnp.where(row == 2, low, 0.0)))
    return x.astype(BF16)


def squares_kernel(key_ref, value_ref, out_ref):
    row = lax.broadcasted_iota(jnp.int32, out_ref.shape, 1)
    out_ref[...] = jnp.where(row == 0, jnp.sum(key_ref[...] * key_ref[...]), jnp.sum(value_ref[...] * value_ref[...]))


def project_kernel(
    latent_hbm, key_hbm, value_hbm, key_proj_hbm, value_proj_hbm, out_ref,
    latent, key, value, key_proj, value_proj, acc_ref, sems,
):
    chunks = sems.shape[0] - 4
    tokens = latent.shape[0] // chunks
    cols = key.shape[1]
    sides = [
        pltpu.make_async_copy(src, dst, sems.at[chunks + i])
        for i, (src, dst) in enumerate((
            (key_hbm, key), (value_hbm, value), (key_proj_hbm, key_proj), (value_proj_hbm, value_proj)
        ))
    ]
    mains = [
        pltpu.make_async_copy(
            latent_hbm.at[pl.ds(i * tokens, tokens)], latent.at[pl.ds(i * tokens, tokens)], sems.at[i]
        )
        for i in range(chunks)
    ]
    for copy in sides[:2] + mains + sides[2:]:
        copy.start()
    sides[0].wait()
    sides[1].wait()
    for i in range(chunks):
        mains[i].wait()
        at = slice(i * tokens, (i + 1) * tokens)
        both = jnp.concatenate([key[at, :], value[at, :]], axis=1)
        part = lax.dot_general(both, latent[at, :], (((0,), (0,)), ((), ())), preferred_element_type=F32)
        acc_ref[...] = part if i == 0 else acc_ref[...] + part
    for which, proj in enumerate((key_proj, value_proj)):
        sides[2 + which].wait()
        high, low = halves(acc_ref[which * cols : (which + 1) * cols])
        p = proj[...]
        r = jnp.dot(high, p, preferred_element_type=F32) + jnp.dot(low, p, preferred_element_type=F32)
        out_ref[which] = r.T.astype(BF16)


def cut_kernel(core_ref, parts_ref, squares_ref, out_ref):
    chips, length, cols = out_ref.shape
    rows = length - TAIL
    mine = parts_ref[:, core_ref[0]].astype(F32).sum(axis=0)
    out_ref[:, :rows] = mine.astype(BF16).reshape(chips, rows, cols)
    squares = jnp.sum(squares_ref[...], axis=0)
    row = lax.broadcasted_iota(jnp.int32, (TAIL, cols), 0)
    key = tail_of(squares[0:1], cols).astype(F32)
    value = tail_of(squares[1:2], cols).astype(F32)
    tail = jnp.where(row < TAIL // 2, key, pltpu.roll(value, TAIL // 2, 0)).astype(BF16)
    for i in range(chips):
        out_ref[i, rows:] = tail


def spread_kernel(pieces_ref, key_ref, value_ref, out_ref, squares_ref):
    rows = pieces_ref.shape[1] - TAIL
    total = jnp.sum(pieces_ref[...].astype(F32), axis=0)
    message = jnp.concatenate(
        [total[:rows].astype(BF16), key_ref[...].astype(BF16), value_ref[...].astype(BF16)], axis=0
    )
    for i in range(out_ref.shape[0]):
        out_ref[i] = message
    key = total[rows : rows + 1] + total[rows + 1 : rows + 2] + total[rows + 2 : rows + 3]
    rows += TAIL // 2
    value = total[rows : rows + 1] + total[rows + 1 : rows + 2] + total[rows + 2 : rows + 3]
    row = lax.broadcasted_iota(jnp.int32, squares_ref.shape, 0)
    squares_ref[...] = jnp.where(row == 0, key, value)


def update_kernel(*refs, rows, weight_rows, entries):
    held, sems = refs[-11:-1], refs[-1]
    inputs, outs = refs[:-21], refs[-21:-11]
    copies = [pltpu.make_async_copy(held[i], outs[i], sems.at[i]) for i in range(len(outs))]
    fill_outputs(*inputs, *held, copies=copies, rows=rows, weight_rows=weight_rows, entries=entries)
    for copy in copies:
        copy.wait()


def fill_outputs(
    place_ref, data_ref, squares_ref, key_w, value_w, key_proj, value_proj, kf, ks, vf, vs,
    key_renewed, value_renewed, key_step, value_step,
    kf_new, ks_new, vf_new, vs_new, key_copy, value_copy,
    *, copies, rows, weight_rows, entries,
):
    own = pl.multiple_of(place_ref[0] * weight_rows, weight_rows)
    cores, chips = data_ref.shape[0], data_ref.shape[1]
    squares = squares_ref[...]
    for which, (w, proj, first, second, renewed, step, first_new, second_new, copy) in enumerate((
        (key_w, key_proj, kf, ks, key_renewed, key_step, kf_new, ks_new, key_copy),
        (value_w, value_proj, vf, vs, value_renewed, value_step, vf_new, vs_new, value_copy),
    )):
        projected = data_ref[which, :, :rows, :].reshape(chips * rows, w.shape[1]).astype(F32)
        fn = FIRST_DECAY * first[...] + (1.0 - FIRST_DECAY) * projected
        sn = SECOND_DECAY * second[...] + (1.0 - SECOND_DECAY) * projected * projected
        first_new[...] = fn
        second_new[...] = sn
        copies[4 + 2 * which].start()
        copies[5 + 2 * which].start()
        pair = jnp.concatenate(halves(fn / (jnp.sqrt(sn) + EPSILON)), axis=1)
        total = squares[which : which + 1]
        scale = LEARN_RATE * jnp.sqrt(total / entries)
        cols = w.shape[1]

        def steps_of(factor):
            r = jnp.dot(factor, pair, preferred_element_type=F32)
            return scale * (r[:, :cols] + r[:, cols:])

        mine = steps_of(proj[pl.ds(own, weight_rows), :])
        step[...] = mine
        renewed[...] = w[...] - mine
        copies[which].start()
        copies[2 + which].start()
        everyone = steps_of(proj[...])
        at = rows + which * weight_rows
        for chip in range(chips):
            for core in range(cores):
                r = ((chip + LEAD) % chips * cores + core) * weight_rows
                old = data_ref[core, chip, at : at + weight_rows, :].astype(F32)
                copy[r : r + weight_rows, :] = (old - everyone[r : r + weight_rows]).astype(BF16)
        copies[8 + which].start()


def swap(a, chips):
    if LEAD == 0:
        return lax.all_to_all(a, Z, 0, 0)
    order = [(i + LEAD) % chips for i in range(chips)]
    return lax.all_to_all(a, Z, 0, 0, axis_index_groups=[order])


def near(a):
    return pltpu.with_memory_space_constraint(a, pltpu.VMEM)


def body(
    latent, key_cotangent, value_cotangent, key_weight, value_weight,
    key_projector, value_projector, key_first, key_second, value_first, value_second,
):
    chips, cores = lax.axis_size(Z), lax.axis_size(CORE)
    columns = lax.axis_size(TP)
    weight_rows, cols = key_weight.shape
    tokens, width = latent.shape
    rank = key_projector.shape[1]
    core = lax.axis_index(CORE).astype(jnp.int32)
    place = lax.axis_index(FS).astype(jnp.int32)
    sds = jax.ShapeDtypeStruct
    smem = pl.BlockSpec(memory_space=pltpu.SMEM)
    vmem = pl.BlockSpec(memory_space=pltpu.VMEM)
    hbm = pl.BlockSpec(memory_space=pl.ANY)

    squares = pl.pallas_call(
        squares_kernel, out_shape=(sds((cores * lax.axis_size(TP[1]), 8, cols), F32),),
        in_specs=[vmem, vmem], out_specs=(vmem,), name="squares",
    )(key_weight, value_weight)[0]
    squares = lax.all_to_all(squares, (CORE, TP[1]), 0, 0)
    parts = pl.pallas_call(
        project_kernel,
        out_shape=(pltpu.VMEM((2, rank, cols), BF16),),
        in_specs=[pl.BlockSpec(memory_space=pl.ANY)] * 5,
        out_specs=(vmem,),
        scratch_shapes=[
            pltpu.VMEM(latent.shape, BF16),
            pltpu.VMEM((tokens, cols), BF16),
            pltpu.VMEM((tokens, cols), BF16),
            pltpu.VMEM((width, rank), BF16),
            pltpu.VMEM((width, rank), BF16),
            pltpu.VMEM((2 * cols, width), F32),
            pltpu.SemaphoreType.DMA((8 + 4,)),
        ],
        name="project",
    )(latent, key_cotangent, value_cotangent, key_projector, value_projector)[0]
    parts = near(lax.all_gather(parts, CORE))

    rows = rank // chips
    pieces = pl.pallas_call(
        cut_kernel, out_shape=(pltpu.VMEM((chips, rows + TAIL, cols), BF16),),
        in_specs=[smem, vmem, vmem], out_specs=(vmem,), name="cut",
    )(core.reshape(1), parts, near(squares))[0]
    pieces = near(swap(pieces, chips))

    length = rows + 2 * weight_rows
    message, squares = pl.pallas_call(
        spread_kernel,
        out_shape=(pltpu.VMEM((chips, length, cols), BF16), pltpu.VMEM((8, cols), F32)),
        in_specs=[vmem] * 3, out_specs=(vmem, vmem), name="spread",
    )(pieces, near(key_weight), near(value_weight))
    message = swap(message, chips)
    squares = lax.psum(squares, TP[0])
    data = near(lax.all_gather(message, CORE))

    entries = float(key_weight.size * chips * cores * columns)
    weight = sds((weight_rows, cols), F32)
    moment = sds((rank, cols), F32)
    copy = sds((width, cols), BF16)

    outs = (weight,) * 4 + (moment,) * 4 + (copy,) * 2

    def update(*refs):
        update_kernel(*refs, rows=rows, weight_rows=weight_rows, entries=entries)

    return pl.pallas_call(
        update,
        out_shape=outs,
        in_specs=[smem] + [vmem] * 10, out_specs=(hbm,) * 10, name="update",
        scratch_shapes=[pltpu.VMEM(o.shape, o.dtype) for o in outs] + [pltpu.SemaphoreType.DMA((len(outs),))],
    )(
        place.reshape(1), data, near(squares), *map(near, (
            key_weight, value_weight, key_projector, value_projector,
            key_first, key_second, value_first, value_second,
        ))
    )


def solution(mesh):
    finer = Mesh(mesh.devices.reshape(16, 2, 8, 4), ("fs_0", "fs_1", "tp_0", "tp_1"))
    return jax.shard_map(
        body,
        mesh=finer,
        in_specs=(P(FS, None),) + (P(FS, TP),) * 4 + (P(),) * 2 + (P(None, TP),) * 4,
        out_specs=(P(FS, TP),) * 4 + (P(None, TP),) * 6,
        check_vma=False,
    )
```
